32 devices in a mesh: sp: 8 (over z, x), tp: 4 (over y, core).
Axes of the slice: x: 2, y: 2, z: 4, core: 2. Of those that a mesh axis runs over, the one named last changes fastest.
Arguments:
- tokens: bfloat16 [2, 1536, 4096], P(None, 'sp', 'tp'), may hold values from -12 to 12
- query_weight: bfloat16 [4096, 2048], P(None, 'tp'), may hold values from -0.09375 to 0.09375
- key_weight: bfloat16 [4096, 2048], P(None, 'tp'), may hold values from -0.09375 to 0.09375
- value_weight: bfloat16 [4096, 2048], P(None, 'tp'), may hold values from -0.09375 to 0.09375
- gate_weight: bfloat16 [4096, 2048], P(None, 'tp'), may hold values from -0.09375 to 0.09375
- beta_weight: bfloat16 [4096, 16], P(None, 'tp'), may hold values from -0.09375 to 0.09375
- decay_weight: bfloat16 [4096, 16], P(None, 'tp'), may hold values from -0.09375 to 0.09375
- beta_bias: float32 [16], P('tp'), may hold values from -6 to -3
- rate_log: float32 [16], P('tp'), may hold values from -12 to -2.5
- out_gain: float32 [128], replicated, may hold values from 0.1 to 1.9
- new_query: bfloat16 [2, 16, 128], P(None, 'tp'), may hold values from -6 to 6
- new_key: bfloat16 [2, 16, 128], P(None, 'tp'), may hold values from -6 to 6
- new_value: bfloat16 [2, 16, 128], P(None, 'tp'), may hold values from -6 to 6
- new_beta: float32 [2, 16], P(None, 'tp'), may hold values from 0.1 to 0.9
- new_decay: float32 [2, 16], P(None, 'tp'), may hold values from 0.3 to 1
Outputs:
- mixed_out: bfloat16 [2, 1536, 2048], P(None, 'sp', 'tp')
- cache: bfloat16 [2, 16, 128, 128], P(None, 'tp', 'sp')
- first_out: float32 [2, 2048], P(None, 'tp')
The draws below stay inside these ranges and needn't reach their ends.
All inputs are finite; a program needn't handle non-finite values.
Results may differ from the reference program's by a relative error of at most 0.0073.
Values may be sent and summed in bfloat16 or wider, within the bound.
A program may use at most 64 MiB of HBM per device.

```python
import jax
import jax.numpy as jnp
from jax import lax

D = 4096
HEADS = 16
HEAD = 128
BLOCK = 64
SEQS = 2
LEN = 1536


def draw_tokens(key, part):
    key_base, key_level, key_common = jax.random.split(key, 3)
    blocks = LEN // BLOCK
    base_draw = jax.random.truncated_normal(key_base, -4.0, 4.0, (SEQS, LEN, D), jnp.float32)
    level_log = jax.random.uniform(key_level, (SEQS, blocks, 1, 1), jnp.float32, -1.0, 1.0)
    common = jnp.zeros((1, 1, D), jnp.float32)
    row_scale = jnp.broadcast_to(jnp.exp(level_log), (SEQS, blocks, BLOCK, 1)).reshape(SEQS, LEN, 1)
    return ((base_draw + common) * row_scale).astype(jnp.bfloat16)


def draw_rate_log(key, part):
    key_slow, key_quick, key_pick = jax.random.split(key, 3)
    slow_rates = jnp.log(jax.random.uniform(key_slow, (HEADS,), jnp.float32, 0.2, 0.6) / LEN)
    quick_rates = jnp.log(jax.random.uniform(key_quick, (HEADS,), jnp.float32, 0.02, 0.06))
    slow_picks = jax.random.randint(key_pick, (HEADS,), 0, 2)
    return jnp.where(slow_picks == 1, slow_rates, quick_rates)


def block_scale(stream_key, shape, shards, low, largest):
    factor_of = 1.0
    for dim, shards_of in shards:
        heights = jax.random.uniform(jax.random.fold_in(jax.random.fold_in(stream_key, 6), dim), (shards_of,), jnp.float32, low / len(shards), largest / len(shards))
        factor_of = factor_of * jnp.repeat(jnp.exp(heights), shape[dim] // shards_of).reshape((-1,) + (1,) * (len(shape) - 1 - dim))
    return factor_of


def centred(key, shape, scale, reach, pieces=(), kind=jnp.bfloat16):
    array = scale * jax.random.normal(key, shape, jnp.float32)
    if pieces:
        array = array * block_scale(key, shape, pieces, -0.22, 0.18)
    return jnp.clip(array, -reach, reach).astype(kind)


def setup_inputs(seed: int = 0) -> dict:
    streams_of = jax.random.split(jax.random.key(seed), 16)
    return {
        "tokens": draw_tokens(jax.random.fold_in(streams_of[15], 71), 0),
        "query_weight": centred(streams_of[1], (D, HEADS * HEAD), D ** -0.5, 0.09375, ((1, 4),)),
        "key_weight": centred(streams_of[2], (D, HEADS * HEAD), D ** -0.5, 0.09375, ((1, 4),)),
        "value_weight": centred(streams_of[3], (D, HEADS * HEAD), D ** -0.5, 0.09375, ((1, 4),)),
        "gate_weight": centred(streams_of[4], (D, HEADS * HEAD), D ** -0.5, 0.09375, ((1, 4),)),
        "beta_weight": centred(streams_of[5], (D, HEADS), D ** -0.5, 0.09375, ((1, 4),)),
        "decay_weight": centred(streams_of[6], (D, HEADS), D ** -0.5, 0.09375, ((1, 4),)),
        "beta_bias": jnp.clip(-6.0 + 3.0 * jax.random.uniform(streams_of[7], (HEADS,), jnp.float32) ** block_scale(streams_of[7], (HEADS,), ((0, 4),), -0.2, 0.2), -6.0, -3.0),
        "rate_log": draw_rate_log(jax.random.fold_in(streams_of[15], 71), 0),
        "out_gain": jnp.clip(1.0 + 0.18 * jax.random.normal(streams_of[9], (HEAD,), jnp.float32), 0.1, 1.9),
        "new_query": centred(streams_of[10], (SEQS, HEADS, HEAD), 1.0, 6.0, ((1, 4),)),
        "new_key": centred(streams_of[11], (SEQS, HEADS, HEAD), 1.0, 6.0, ((1, 4),)),
        "new_value": centred(streams_of[12], (SEQS, HEADS, HEAD), 1.0, 6.0, ((1, 4),)),
        "new_beta": jnp.clip(0.1 + 0.79999997 * jax.random.uniform(streams_of[13], (SEQS, HEADS), jnp.float32) ** block_scale(streams_of[13], (SEQS, HEADS), ((1, 4),), -0.2, 0.2), 0.1, 0.9),
        "new_decay": jnp.clip(0.3 + 0.7 * jax.random.uniform(streams_of[14], (SEQS, HEADS), jnp.float32) ** block_scale(streams_of[14], (SEQS, HEADS), ((1, 4),), -0.2, 0.2), 0.3, 1.0),
    }


unit_floor = 1.0
norm_floor = 0.001
highest = lax.Precision.HIGHEST

def matmul(form, left, right):
    return jnp.einsum(form, left, right, precision=highest)

def unit_rows(values):
    return values * lax.rsqrt(lax.optimization_barrier(jnp.sum(values * values, axis=-1, keepdims=True)) + unit_floor)

def head_norm(values, out_gain):
    return values * lax.rsqrt(lax.optimization_barrier(jnp.mean(values * values, axis=-1, keepdims=True)) + norm_floor) * out_gain

def stored(values):
    return lax.optimization_barrier(values.astype(jnp.bfloat16)).astype(jnp.float32)

def unit_lower_inverse(lower_part):
    extent = lower_part.shape[-1]
    nilpotent = -lower_part
    inverse = jnp.eye(extent, dtype=jnp.float32) + nilpotent
    for _ in range(extent.bit_length() - 2):
        nilpotent = matmul('...ij,...jk->...ik', nilpotent, nilpotent)
        inverse = inverse + matmul('...ij,...jk->...ik', nilpotent, inverse)
    return inverse

def prepare(query_rows, key_rows, value_rows, beta_in, decay_in, beta_bias, rate_log, seq_count, length, head_count):
    extent = query_rows.shape[-1] // head_count
    blocks = length // BLOCK

    def by_head(values):
        shaped = values.reshape(seq_count, blocks, BLOCK, head_count, extent)
        return shaped.transpose(0, 3, 1, 2, 4).reshape(seq_count * head_count, blocks, BLOCK, extent)

    def by_scalar(values):
        shaped = values.reshape(seq_count, blocks, BLOCK, head_count)
        return shaped.transpose(0, 3, 1, 2).reshape(seq_count * head_count, blocks, BLOCK)
    queries = unit_rows(by_head(query_rows))
    key_unit = unit_rows(by_head(key_rows))
    values = by_head(value_rows)
    strength = by_scalar(jax.nn.sigmoid(beta_in + beta_bias))
    decays = by_scalar(-jnp.exp(rate_log) * jax.nn.softplus(decay_in))
    return (queries, key_unit, values, strength, decays)

def block_terms(queries, key_unit, values, strength, decays):
    extent = decays.shape[-1]
    cumulative = jnp.cumsum(decays, axis=-1)
    causal = jnp.tril(jnp.ones((extent, extent), bool))
    strict = jnp.tril(jnp.ones((extent, extent), bool), -1)
    spread = cumulative[..., :, None] - cumulative[..., None, :]
    weights = jnp.where(causal, jnp.exp(jnp.where(causal, spread, 0.0)), 0.0)
    key_beta = key_unit * strength[..., None]
    lower_part = jnp.where(strict, matmul('...td,...sd->...ts', key_beta, key_unit) * weights, 0.0)
    inverse = unit_lower_inverse(lower_part)
    update = matmul('...ts,...se->...te', inverse, values * strength[..., None])
    carry_w = matmul('...ts,...sd->...td', inverse, key_beta * jnp.exp(cumulative)[..., None])
    scores = matmul('...td,...sd->...ts', queries, key_unit) * weights
    query_decay = queries * jnp.exp(cumulative)[..., None]
    last_log = cumulative[..., -1]
    key_decay = key_unit * jnp.exp(last_log[..., None] - cumulative)[..., None]
    return (update, carry_w, query_decay, scores, key_decay, last_log)

def first_read(cache_whole, new_query, new_key, new_value, new_beta, new_decay, out_gain):
    seq_count, head_count, extent, _ = cache_whole.shape
    memory = lax.optimization_barrier(cache_whole).astype(jnp.float32)
    query_unit = unit_rows(new_query.astype(jnp.float32))
    key_unit = unit_rows(new_key.astype(jnp.float32))
    recall = matmul('shde,shd->she', memory, query_unit)
    retrieve = matmul('shde,shd->she', memory, key_unit)
    intersect = lax.optimization_barrier(jnp.sum(key_unit * query_unit, axis=-1))
    fresh_values = new_value.astype(jnp.float32) - new_decay[..., None] * retrieve
    read_heads = new_decay[..., None] * recall + (new_beta * intersect)[..., None] * fresh_values
    return head_norm(read_heads, out_gain).reshape(seq_count, head_count * extent)

def reference(tokens, query_weight, key_weight, value_weight, gate_weight, beta_weight, decay_weight, beta_bias, rate_log, out_gain, new_query, new_key, new_value, new_beta, new_decay):
    flat_rows = tokens.reshape(SEQS * LEN, D)

    def project(weight):
        return jnp.dot(flat_rows, weight, preferred_element_type=jnp.float32)
    query_rows = stored(project(query_weight))
    key_rows = stored(project(key_weight))
    value_rows = stored(project(value_weight))
    gate_rows = stored(project(gate_weight))
    beta_in = project(beta_weight)
    decay_in = project(decay_weight)
    prepared = prepare(query_rows, key_rows, value_rows, beta_in, decay_in, beta_bias, rate_log, SEQS, LEN, HEADS)
    block_data = block_terms(*prepared)

    def advance(state_now, inputs):
        update, carry_w, query_decay, scores, key_decay, last_log = inputs
        fresh_values = update - matmul('btd,bde->bte', carry_w, state_now)
        block_out = matmul('btd,bde->bte', query_decay, state_now) + matmul('bts,bse->bte', scores, fresh_values)
        state_next = state_now * jnp.exp(last_log)[:, None, None] + matmul('bsd,bse->bde', key_decay, fresh_values)
        return (state_next, block_out)
    inputs = tuple((jnp.moveaxis(member, 1, 0) for member in block_data))
    batch_size = SEQS * HEADS
    final_state, outputs = lax.scan(advance, jnp.zeros((batch_size, HEAD, HEAD), jnp.float32), inputs)
    heads_out = outputs.reshape(LEN // BLOCK, SEQS, HEADS, BLOCK, HEAD).transpose(1, 0, 3, 2, 4)
    heads_out = heads_out.reshape(SEQS, LEN, HEADS, HEAD)
    gate_values = gate_rows.reshape(SEQS, LEN, HEADS, HEAD)
    mixed_out = (head_norm(heads_out, out_gain) * jax.nn.silu(gate_values)).astype(jnp.bfloat16)
    mixed_out = mixed_out.reshape(SEQS, LEN, HEADS * HEAD)
    cache = final_state.reshape(SEQS, HEADS, HEAD, HEAD).astype(jnp.bfloat16)
    first_out = first_read(cache, new_query, new_key, new_value, new_beta, new_decay, out_gain)
    return (mixed_out, cache, first_out)
```

```python
import functools

import jax
import jax.numpy as jnp
from jax import lax
from jax.experimental import pallas as pl
from jax.experimental.pallas import tpu as pltpu
from jax.sharding import PartitionSpec as P

unit_floor = 1.0
norm_floor = 0.001
highest = lax.Precision.HIGHEST
MESH = pl.DeviceIdType.MESH
PAD = 8
f32 = jnp.float32
bf16 = jnp.bfloat16

NN = (((1,), (0,)), ((), ()))
NT = (((1,), (1,)), ((), ()))
TN = (((0,), (0,)), ((), ()))


def dot(left, right, dims=NN, precision=None):
    return lax.dot_general(left, right, dims, precision=precision, preferred_element_type=f32)


def gather_kernel(
    n, seqs, x_ref, wq_ref, wk_ref, wv_ref, wg_ref, bd_ref, out_ref, small_ref,
    xs, wbuf, acc, sacc, wsem, cross_sem, part_sem, fwd_sem, rx,
):
    me = lax.axis_index("tp")
    y, c = me // 2, lax.rem(me, 2)
    chips = n // 2
    rows, kd = x_ref.shape
    span = rows // seqs
    _, chunks, _, kc = xs.shape
    partner = y * 2 + (1 - c)
    weights = (wq_ref, wk_ref, wv_ref, wg_ref)

    barrier = pltpu.get_barrier_semaphore()
    pl.semaphore_signal(barrier, inc=1, device_id={"tp": partner}, device_id_type=MESH)
    for d in range(1, chips):
        to = lax.rem(y + d, chips) * 2 + c
        pl.semaphore_signal(barrier, inc=1, device_id={"tp": to}, device_id_type=MESH)

    order = [me, partner]
    for d in range(1, chips):
        source = lax.rem(y - d + chips, chips)
        order += [source * 2 + c, source * 2 + (1 - c)]

    def weight_copy(w, slot):
        start = pl.multiple_of(order[slot] * kd, kd)
        return pltpu.make_async_copy(
            weights[w].at[pl.ds(start, kd), :], wbuf.at[w, slot], wsem.at[w, slot]
        )

    for slot in range(n):
        for w in range(4):
            weight_copy(w, slot).start()
    pl.semaphore_wait(barrier, chips)

    def cols(ck):
        return pl.ds(ck * kc, kc)

    def cross_copy(d, ck):
        to = lax.rem(y + d, chips) * 2 + c
        return pltpu.make_async_remote_copy(
            src_ref=x_ref.at[:, cols(ck)], dst_ref=xs.at[me, ck],
            send_sem=cross_sem.at[d - 1, ck], recv_sem=rx.at[me, ck],
            device_id={"tp": to}, device_id_type=MESH,
        )

    def part_copy(ck):
        return pltpu.make_async_remote_copy(
            src_ref=x_ref.at[:, cols(ck)], dst_ref=xs.at[me, ck],
            send_sem=part_sem.at[ck], recv_sem=rx.at[me, ck],
            device_id={"tp": partner}, device_id_type=MESH,
        )

    def fwd_copy(d, ck):
        b = order[2 * d]
        return pltpu.make_async_remote_copy(
            src_ref=xs.at[b, ck], dst_ref=xs.at[b, ck],
            send_sem=fwd_sem.at[d - 1, ck], recv_sem=rx.at[b, ck],
            device_id={"tp": partner}, device_id_type=MESH,
        )

    def arrive(b, ck):
        pltpu.make_async_remote_copy(
            src_ref=xs.at[b, ck], dst_ref=xs.at[b, ck],
            send_sem=part_sem.at[ck], recv_sem=rx.at[b, ck],
            device_id={"tp": partner}, device_id_type=MESH,
        ).wait_recv()

    for ck in range(chunks):
        for d in range(1, chips):
            cross_copy(d, ck).start()
    for ck in range(chunks):
        part_copy(ck).start()

    def small(x, start, depth, first):
        piece = bd_ref[:, pl.ds(pl.multiple_of(start, depth), depth)]
        for s in range(seqs):
            term = dot(piece, x[s * span : (s + 1) * span], NT)
            sacc[s] = term if first else sacc[s] + term

    for w in range(4):
        weight_copy(w, 0).wait()
        acc[w] = dot(x_ref[...], wbuf[w, 0])
    small(x_ref[...], me * kd, kd, True)

    def use(slot, ck):
        b = order[slot]
        x = xs[b, ck]
        for w in range(4):
            if ck == 0:
                weight_copy(w, slot).wait()
            acc[w] += dot(x, wbuf[w, slot, pl.ds(ck * kc, kc), :])
        small(x, b * kd + ck * kc, kc, False)

    for ck in range(chunks):
        arrive(partner, ck)
        use(1, ck)
    for d in range(1, chips):
        for ck in range(chunks):
            arrive(order[2 * d], ck)
            fwd_copy(d, ck).start()
            use(2 * d, ck)
            arrive(order[2 * d + 1], ck)
            use(2 * d + 1, ck)
    for w in range(4):
        out_ref[w] = acc[w].astype(bf16)
    small_ref[...] = sacc[...]
    for ck in range(chunks):
        part_copy(ck).wait_send()
        for d in range(1, chips):
            cross_copy(d, ck).wait_send()
            fwd_copy(d, ck).wait_send()


def gather_project(n, seqs, tokens, weights, bd):
    rows, kd = tokens.shape
    width = weights[0].shape[1]
    kc = 256 if kd % 256 == 0 else kd
    chunks = kd // kc
    chips = n // 2
    span = rows // seqs
    return pl.pallas_call(
        functools.partial(gather_kernel, n, seqs),
        out_shape=(
            jax.ShapeDtypeStruct((4, rows, width), bf16),
            jax.ShapeDtypeStruct((seqs, 2 * PAD, span), f32),
        ),
        in_specs=[pl.BlockSpec(memory_space=pltpu.VMEM)]
        + [pl.BlockSpec(memory_space=pl.ANY)] * 4
        + [pl.BlockSpec(memory_space=pltpu.VMEM)],
        out_specs=(pl.BlockSpec(memory_space=pltpu.VMEM),) * 2,
        scratch_shapes=[
            pltpu.VMEM((n, chunks, rows, kc), bf16),
            pltpu.VMEM((4, n, kd, width), bf16),
            pltpu.VMEM((4, rows, width), f32),
            pltpu.VMEM((seqs, 2 * PAD, span), f32),
            pltpu.SemaphoreType.DMA((4, n)),
            pltpu.SemaphoreType.DMA((chips - 1, chunks)),
            pltpu.SemaphoreType.DMA((chunks,)),
            pltpu.SemaphoreType.DMA((chips - 1, chunks)),
            pltpu.SemaphoreType.DMA((n, chunks)),
        ],
        compiler_params=pltpu.CompilerParams(
            collective_id=0, has_side_effects=True, vmem_limit_bytes=60 * 1024 * 1024
        ),
    )(tokens, *weights, bd)


def unit_rows(values):
    return values * lax.rsqrt(jnp.sum(values * values, axis=-1, keepdims=True) + unit_floor)


def delta_kernel(
    n, seqs, heads, group, rows_ref, small_ref, par_ref, gain_ref, nq_ref, nk_ref, nv_ref,
    nb_ref, nd_ref, mixed_ref, cache_ref, first_ref,
    cum_row, cum_col, beta_col, local_out, reach, out_box, in_box, back_out, back_in, tail_out,
    tail_in, send1, recv1, send2, recv2, send3, recv3,
):
    me = lax.axis_index("sp")
    pairs = seqs * heads
    span = rows_ref.shape[1] // seqs
    extent = rows_ref.shape[2] // heads
    key_rows = extent // n

    barrier = pltpu.get_barrier_semaphore()
    for d in range(1, n):
        to = lax.rem(me + d, n)
        pl.semaphore_signal(barrier, inc=1, device_id={"sp": to}, device_id_type=MESH)

    row = lax.broadcasted_iota(jnp.int32, (span, span), 0)
    col = lax.broadcasted_iota(jnp.int32, (span, span), 1)
    upper = jnp.where(row <= col, 1.0, 0.0)
    bias, rate = par_ref[0:PAD], par_ref[PAD : 2 * PAD]
    for s in range(seqs):
        beta = jax.nn.sigmoid(small_ref[s, 0:PAD, :] + bias)
        pre = small_ref[s, PAD : 2 * PAD, :]
        soft = jnp.maximum(pre, 0.0) + jnp.log1p(jnp.exp(-jnp.abs(pre)))
        cum = dot(-jnp.exp(rate) * soft, upper, NN, highest)
        cum_row[s] = cum
        cum_col[s] = cum.T
        beta_col[s] = beta.T
    eye_lane = lax.broadcasted_iota(jnp.int32, (extent, extent), 0) == lax.broadcasted_iota(
        jnp.int32, (extent, extent), 1
    )
    pl.semaphore_wait(barrier, n - 1)

    def send_box(p):
        return pltpu.make_async_remote_copy(
            src_ref=out_box.at[p], dst_ref=in_box.at[me],
            send_sem=send1.at[p], recv_sem=recv1.at[me],
            device_id={"sp": p}, device_id_type=MESH,
        )

    def local_group(i, _):
        ps = [lax.rem(me + 1 + i * group + j, pairs) for j in range(group)]
        each = []
        for p in ps:
            s, h = p // heads, lax.rem(p, heads)
            at = pl.ds(pl.multiple_of(s * span, span), span)
            lanes = pl.ds(pl.multiple_of(h * extent, extent), extent)
            q = unit_rows(rows_ref[0, at, lanes].astype(f32))
            k = unit_rows(rows_ref[1, at, lanes].astype(f32))
            v = rows_ref[2, at, lanes].astype(f32)
            pick = lax.broadcasted_iota(jnp.int32, (span, PAD), 1) == h
            cumc = jnp.sum(jnp.where(pick, cum_col[s], 0.0), axis=1, keepdims=True)
            beta = jnp.sum(jnp.where(pick, beta_col[s], 0.0), axis=1, keepdims=True)
            cumr = cum_row[s, pl.ds(h, 1), :]
            causal = row >= col
            weights = jnp.where(causal, jnp.exp(jnp.where(causal, cumc - cumr, 0.0)), 0.0)
            kb = k * beta
            kh = k.astype(bf16)
            lower = jnp.where(row > col, dot(kb.astype(bf16), kh, NT) * weights, 0.0)
            score = (dot(q.astype(bf16), kh, NT) * weights).astype(bf16)
            grow = jnp.exp(cumc)
            right = jnp.concatenate([v * beta, kb * grow], axis=1).astype(bf16)
            last = cumc[span - 1 :, :]
            kdec = (k * jnp.exp(last - cumc)).astype(bf16)
            each.append([lower, score, right, kdec, q * grow, jnp.exp(last)])
        unit = jnp.where(row == col, 1.0, 0.0)
        pair_mask = ((row >> 1) == (col >> 1)) & (row > col)
        inv = [unit - jnp.where(pair_mask, e[0], 0.0) for e in each]
        level = 1
        while (1 << level) < span:
            mask = ((row >> (level + 1)) == (col >> (level + 1))) & ((row >> level) > (col >> level))
            inv_h = [m.astype(bf16) for m in inv]
            mid = [
                dot(jnp.where(mask, e[0], 0.0).astype(bf16), m).astype(bf16)
                for e, m in zip(each, inv_h)
            ]
            inv = [m - dot(mh, t) for m, mh, t in zip(inv, inv_h, mid)]
            level += 1
        uw = [dot(m.astype(bf16), e[2]).astype(bf16) for m, e in zip(inv, each)]
        out = [dot(e[1], u) for e, u in zip(each, uw)]
        fin = [dot(e[3], u, TN) for e, u in zip(each, uw)]
        for p, e, o, z in zip(ps, each, out, fin):
            local_out[p] = o[:, :extent]
            reach[p] = (e[4] - o[:, extent:]).astype(bf16)
            step = (jnp.where(eye_lane, e[5] - 1.0, 0.0) - z[:, extent:]).astype(bf16)
            state = z[:, :extent].astype(bf16)

            @pl.when(p == me)
            def _():
                in_box[me, 0] = step
                in_box[me, 1] = state

            @pl.when(p != me)
            def _():
                out_box[p, 0] = step
                out_box[p, 1] = state
                send_box(p).start()

        return 0

    lax.fori_loop(0, pairs // group, local_group, 0)

    def back_copy(j):
        return pltpu.make_async_remote_copy(
            src_ref=back_out.at[j], dst_ref=back_in.at[me],
            send_sem=send2.at[j], recv_sem=recv2.at[me],
            device_id={"sp": j}, device_id_type=MESH,
        )

    def tail_copy(j):
        return pltpu.make_async_remote_copy(
            src_ref=tail_out.at[j], dst_ref=tail_in.at[me],
            send_sem=send3.at[j], recv_sem=recv3.at[me],
            device_id={"sp": j}, device_id_type=MESH,
        )

    @pl.when(me < pairs)
    def _():
        def chain(j, state):
            half = state.astype(bf16)

            @pl.when(j == me)
            def _():
                back_in[me] = half

            @pl.when(j != me)
            def _():
                back_out[j] = half
                back_copy(j).start()
                pltpu.make_async_remote_copy(
                    src_ref=out_box.at[0], dst_ref=in_box.at[j],
                    send_sem=send1.at[0], recv_sem=recv1.at[j],
                    device_id={"sp": j}, device_id_type=MESH,
                ).wait_recv()

            return state + dot(in_box[j, 0], half) + in_box[j, 1].astype(f32)

        final = lax.fori_loop(0, n, chain, jnp.zeros((extent, extent), f32))
        memory = final.astype(bf16).astype(f32)
        shape3 = nq_ref.shape
        mine = (
            lax.broadcasted_iota(jnp.int32, shape3, 0) * heads
            + lax.broadcasted_iota(jnp.int32, shape3, 1)
        ) == me

        def own(ref):
            kept = jnp.where(mine, ref[...].astype(f32), 0.0)
            return jnp.sum(jnp.sum(kept, axis=0), axis=0, keepdims=True)

        qn, kn = unit_rows(own(nq_ref)), unit_rows(own(nk_ref))
        both = jnp.concatenate([jnp.broadcast_to(qn, (PAD, extent)), jnp.broadcast_to(kn, (PAD, extent))], axis=0)
        reads = dot(both, memory, NN, highest)
        recall, retrieve = reads[0:1], reads[PAD : PAD + 1]
        s, h = me // heads, lax.rem(me, heads)
        beta_new, decay_new = nb_ref[s, h], nd_ref[s, h]
        fresh = own(nv_ref) - decay_new * retrieve
        meet = jnp.sum(kn * qn, axis=-1, keepdims=True)
        read = decay_new * recall + (beta_new * meet) * fresh
        norm = lax.rsqrt(jnp.mean(read * read, axis=-1, keepdims=True) + norm_floor)
        answer = jnp.broadcast_to(read * norm * gain_ref[...], (PAD, extent))
        for j in range(n):
            tail_out[j, 0:key_rows, :] = memory[j * key_rows : (j + 1) * key_rows]
            tail_out[j, tail_out.shape[1] - PAD :, :] = answer

        def push(j, _):
            @pl.when(j == me)
            def _():
                tail_in[me] = tail_out[me]

            @pl.when(j != me)
            def _():
                tail_copy(j).start()

            return 0

        lax.fori_loop(0, n, push, 0)

    gain = gain_ref[...]

    def finish(i, _):
        p = lax.rem(me + i, pairs)
        s, h = p // heads, lax.rem(p, heads)
        at = pl.ds(pl.multiple_of(s * span, span), span)
        lanes = pl.ds(pl.multiple_of(h * extent, extent), extent)

        @pl.when(p != me)
        def _():
            pltpu.make_async_remote_copy(
                src_ref=back_out.at[0], dst_ref=back_in.at[p],
                send_sem=send2.at[0], recv_sem=recv2.at[p],
                device_id={"sp": p}, device_id_type=MESH,
            ).wait_recv()

        o = local_out[p] + dot(reach[p], back_in[p])
        norm = lax.rsqrt(jnp.mean(o * o, axis=-1, keepdims=True) + norm_floor)
        gate = rows_ref[3, at, lanes].astype(f32)
        mixed_ref[at, lanes] = (o * norm * gain * (gate * jax.nn.sigmoid(gate))).astype(bf16)
        return 0

    lax.fori_loop(0, pairs, finish, 0)

    for p in range(pairs):

        @pl.when(p != me)
        def _():
            pltpu.make_async_remote_copy(
                src_ref=tail_out.at[0], dst_ref=tail_in.at[p],
                send_sem=send3.at[0], recv_sem=recv3.at[p],
                device_id={"sp": p}, device_id_type=MESH,
            ).wait_recv()

        cache_ref[p] = tail_in[p, 0:key_rows, :].astype(bf16)
        last = tail_in.shape[1]
        first_ref[p : p + 1, :] = tail_in[p, last - PAD : last - PAD + 1, :]

    for p in range(pairs):

        @pl.when(p != me)
        def _():
            send_box(p).wait_send()

    @pl.when(me < pairs)
    def _():
        for j in range(n):

            @pl.when(j != me)
            def _():
                back_copy(j).wait_send()
                tail_copy(j).wait_send()


def delta(n, seqs, heads, rows4, small, par, gain, nq, nk, nv, nb, nd):
    _, rows, width = rows4.shape
    span, extent = rows // seqs, width // heads
    pairs = seqs * heads
    key_rows = extent // n
    tail = -(-key_rows // PAD) * PAD + PAD
    vmem = pl.BlockSpec(memory_space=pltpu.VMEM)
    smem = pl.BlockSpec(memory_space=pltpu.SMEM)
    return pl.pallas_call(
        functools.partial(delta_kernel, n, seqs, heads, 2),
        out_shape=(
            jax.ShapeDtypeStruct((rows, width), bf16),
            jax.ShapeDtypeStruct((pairs, key_rows, extent), bf16),
            jax.ShapeDtypeStruct((pairs, extent), f32),
        ),
        in_specs=[vmem] * 7 + [smem] * 2,
        out_specs=(vmem,) * 3,
        scratch_shapes=[
            pltpu.VMEM((seqs, PAD, span), f32),
            pltpu.VMEM((seqs, span, PAD), f32),
            pltpu.VMEM((seqs, span, PAD), f32),
            pltpu.VMEM((pairs, span, extent), f32),
            pltpu.VMEM((pairs, span, extent), bf16),
            pltpu.VMEM((pairs, 2, extent, extent), bf16),
            pltpu.VMEM((n, 2, extent, extent), bf16),
            pltpu.VMEM((n, extent, extent), bf16),
            pltpu.VMEM((pairs, extent, extent), bf16),
            pltpu.VMEM((n, tail, extent), f32),
            pltpu.VMEM((pairs, tail, extent), f32),
            pltpu.SemaphoreType.DMA((pairs,)),
            pltpu.SemaphoreType.DMA((n,)),
            pltpu.SemaphoreType.DMA((n,)),
            pltpu.SemaphoreType.DMA((pairs,)),
            pltpu.SemaphoreType.DMA((n,)),
            pltpu.SemaphoreType.DMA((pairs,)),
        ],
        compiler_params=pltpu.CompilerParams(
            collective_id=1, has_side_effects=True, vmem_limit_bytes=48 * 1024 * 1024
        ),
    )(rows4, small, par, gain, nq, nk, nv, nb, nd)


def shards(
    tokens, query_weight, key_weight, value_weight, gate_weight, beta_weight, decay_weight,
    beta_bias, rate_log, out_gain, new_query, new_key, new_value, new_beta, new_decay,
):
    seqs, span, kd = tokens.shape
    heads = rate_log.shape[0]
    extent = out_gain.shape[0]
    tp, sp = lax.axis_size("tp"), lax.axis_size("sp")
    fill = ((0, PAD - heads), (0, 0))
    bd = jnp.concatenate([jnp.pad(beta_weight.T, fill), jnp.pad(decay_weight.T, fill)], axis=0)
    par = jnp.concatenate(
        [jnp.pad(beta_bias[:, None], fill), jnp.pad(rate_log[:, None], fill)], axis=0
    )
    weights = (query_weight, key_weight, value_weight, gate_weight)
    rows4, small = gather_project(tp, seqs, tokens.reshape(seqs * span, kd), weights, bd)
    mixed, cache, first = delta(
        sp, seqs, heads, rows4, small, par, out_gain[None], new_query, new_key, new_value,
        new_beta, new_decay,
    )
    return (
        mixed.reshape(seqs, span, heads * extent),
        cache.reshape(seqs, heads, extent // sp, extent),
        first.reshape(seqs, heads * extent),
    )


def solution(mesh):
    placed = (
        P(None, "sp", "tp"),
        P(None, "tp"),
        P(None, "tp"),
        P(None, "tp"),
        P(None, "tp"),
        P(None, "tp"),
        P(None, "tp"),
        P("tp"),
        P("tp"),
        P(),
        P(None, "tp", None),
        P(None, "tp", None),
        P(None, "tp", None),
        P(None, "tp"),
        P(None, "tp"),
    )
    return jax.shard_map(
        shards,
        mesh=mesh,
        in_specs=placed,
        out_specs=(P(None, "sp", "tp"), P(None, "tp", "sp", None), P(None, "tp")),
        check_vma=False,
    )
```

```python
import functools

import jax
import jax.numpy as jnp
from jax import lax
from jax.experimental import pallas as pl
from jax.experimental.pallas import tpu as pltpu
from jax.sharding import PartitionSpec as P

unit_floor = 1.0
norm_floor = 0.001
highest = lax.Precision.HIGHEST
MESH = pl.DeviceIdType.MESH
PAD = 8
f32 = jnp.float32
bf16 = jnp.bfloat16

NN = (((1,), (0,)), ((), ()))
NT = (((1,), (1,)), ((), ()))
TN = (((0,), (0,)), ((), ()))


def dot(left, right, dims=NN, precision=None):
    return lax.dot_general(left, right, dims, precision=precision, preferred_element_type=f32)


def unit_rows(values):
    return values * lax.rsqrt(jnp.sum(values * values, axis=-1, keepdims=True) + unit_floor)


def kernel(
    n, tp, group,
    x_hbm, wq_ref, wk_ref, wv_ref, wg_ref, bw_ref, dw_ref, bias_ref, rate_ref, gain_ref, nq_ref,
    nk_ref, nv_ref, nb_ref, nd_ref, mixed_ref, cache_ref, first_ref,
    x_ref, xs, wbuf, acc, sacc, bd, rows_ref,
    cum_row, cum_col, beta_col, local_out, reach, out_box, in_box, back_out, back_in, tail_out,
    tail_in, xsem, wsem, cross_sem, part_sem, fwd_sem, rx, send1, recv1, send2, recv2, send3, recv3,
):
    me = lax.axis_index("sp")
    seqs, span, kd = x_hbm.shape
    heads, = bias_ref.shape
    pairs = seqs * heads
    extent = rows_ref.shape[2] // heads
    key_rows = extent // n
    rank = lax.axis_index("tp")
    y, c = rank // 2, lax.rem(rank, 2)
    chips = tp // 2
    _, _, chunks, _, kc = xs.shape
    partner = y * 2 + (1 - c)
    big = (wq_ref, wk_ref, wv_ref, wg_ref)

    barrier = pltpu.get_barrier_semaphore()
    pl.semaphore_signal(barrier, inc=1, device_id={"tp": partner}, device_id_type=MESH)
    for d in range(1, chips):
        to = lax.rem(y + d, chips) * 2 + c
        pl.semaphore_signal(barrier, inc=1, device_id={"tp": to}, device_id_type=MESH)
    for d in range(1, n):
        to = lax.rem(me + d, n)
        pl.semaphore_signal(barrier, inc=1, device_id={"sp": to}, device_id_type=MESH)

    order = [rank, partner]
    for d in range(1, chips):
        source = lax.rem(y - d + chips, chips)
        order += [source * 2 + c, source * 2 + (1 - c)]

    def token_copy(s):
        return pltpu.make_async_copy(x_hbm.at[s], x_ref.at[s], xsem.at[s])

    def weight_copy(w, slot):
        start = pl.multiple_of(order[slot] * kd, kd)
        return pltpu.make_async_copy(
            big[w].at[pl.ds(start, kd), :], wbuf.at[w, slot], wsem.at[w, slot]
        )

    for s in range(seqs):
        token_copy(s).start()
    for slot in range(tp):
        for w in range(4):
            weight_copy(w, slot).start()
    bd[...] = jnp.zeros_like(bd)
    bd[0:heads] = bw_ref[...]
    bd[PAD : PAD + heads] = dw_ref[...]

    def cols(ck):
        return pl.ds(ck * kc, kc)

    def cross_copy(d, s, ck):
        to = lax.rem(y + d, chips) * 2 + c
        return pltpu.make_async_remote_copy(
            src_ref=x_ref.at[s, :, cols(ck)], dst_ref=xs.at[rank, s, ck],
            send_sem=cross_sem.at[d - 1, s, ck], recv_sem=rx.at[rank, s, ck],
            device_id={"tp": to}, device_id_type=MESH,
        )

    def part_copy(s, ck):
        return pltpu.make_async_remote_copy(
            src_ref=x_ref.at[s, :, cols(ck)], dst_ref=xs.at[rank, s, ck],
            send_sem=part_sem.at[s, ck], recv_sem=rx.at[rank, s, ck],
            device_id={"tp": partner}, device_id_type=MESH,
        )

    def fwd_copy(d, s, ck):
        b = order[2 * d]
        return pltpu.make_async_remote_copy(
            src_ref=xs.at[b, s, ck], dst_ref=xs.at[b, s, ck],
            send_sem=fwd_sem.at[d - 1, s, ck], recv_sem=rx.at[b, s, ck],
            device_id={"tp": partner}, device_id_type=MESH,
        )

    def arrive(b, s, ck):
        pltpu.make_async_remote_copy(
            src_ref=xs.at[b, s, ck], dst_ref=xs.at[b, s, ck],
            send_sem=part_sem.at[s, ck], recv_sem=rx.at[b, s, ck],
            device_id={"tp": partner}, device_id_type=MESH,
        ).wait_recv()

    token_copy(0).wait()
    pl.semaphore_wait(barrier, chips + n - 1)
    for s in range(seqs):
        if s:
            token_copy(s).wait()
        for ck in range(chunks):
            for d in range(1, chips):
                cross_copy(d, s, ck).start()
    for s in range(seqs):
        for ck in range(chunks):
            part_copy(s, ck).start()

    row = lax.broadcasted_iota(jnp.int32, (span, span), 0)
    col = lax.broadcasted_iota(jnp.int32, (span, span), 1)
    eye_lane = lax.broadcasted_iota(jnp.int32, (extent, extent), 0) == lax.broadcasted_iota(
        jnp.int32, (extent, extent), 1
    )
    slot_of = lax.broadcasted_iota(jnp.int32, (PAD, 1), 0)
    bias = jnp.zeros((PAD, 1), f32)
    rate = jnp.zeros((PAD, 1), f32)
    for h in range(heads):
        bias = jnp.where(slot_of == h, bias_ref[h], bias)
        rate = jnp.where(slot_of == h, rate_ref[h], rate)

    def small(x, s, start, depth, first):
        term = dot(bd[:, pl.ds(pl.multiple_of(start, depth), depth)], x, NT)
        sacc[s] = term if first else sacc[s] + term

    def at_rows(s):
        return pl.ds(s * span, span)

    for w in range(4):
        weight_copy(w, 0).wait()
        for s in range(seqs):
            acc[w, at_rows(s)] = dot(x_ref[s], wbuf[w, 0])
    for s in range(seqs):
        small(x_ref[s], s, rank * kd, kd, True)

    def use(slot, s, ck):
        b = order[slot]
        x = xs[b, s, ck]
        for w in range(4):
            if ck == 0 and s == 0:
                weight_copy(w, slot).wait()
            acc[w, at_rows(s)] += dot(x, wbuf[w, slot, pl.ds(ck * kc, kc), :])
        small(x, s, b * kd + ck * kc, kc, False)

    for s in range(seqs):
        for ck in range(chunks):
            arrive(partner, s, ck)
            use(1, s, ck)

    def project(s):
        for d in range(1, chips):
            for ck in range(chunks):
                arrive(order[2 * d], s, ck)
                fwd_copy(d, s, ck).start()
                use(2 * d, s, ck)
                arrive(order[2 * d + 1], s, ck)
                use(2 * d + 1, s, ck)
        for w in range(4):
            rows_ref[w, at_rows(s)] = acc[w, at_rows(s)].astype(bf16)
        beta = jax.nn.sigmoid(sacc[s, 0:PAD, :] + bias)
        pre = sacc[s, PAD : 2 * PAD, :]
        soft = jnp.maximum(pre, 0.0) + jnp.log1p(jnp.exp(-jnp.abs(pre)))
        cum = dot(-jnp.exp(rate) * soft, jnp.where(row <= col, 1.0, 0.0), NN, highest)
        cum_row[s] = cum
        cum_col[s] = cum.T
        beta_col[s] = beta.T

    def send_box(p):
        return pltpu.make_async_remote_copy(
            src_ref=out_box.at[p], dst_ref=in_box.at[me],
            send_sem=send1.at[p], recv_sem=recv1.at[me],
            device_id={"sp": p}, device_id_type=MESH,
        )

    def local_group(s0, i, _):
        ps = [s0 * heads + lax.rem(me + 1 + i * group + j, heads) for j in range(group)]
        each = []
        for p in ps:
            s, h = s0, lax.rem(p, heads)
            at = at_rows(s)
            lanes = pl.ds(pl.multiple_of(h * extent, extent), extent)
            q = unit_rows(rows_ref[0, at, lanes].astype(f32))
            k = unit_rows(rows_ref[1, at, lanes].astype(f32))
            v = rows_ref[2, at, lanes].astype(f32)
            pick = lax.broadcasted_iota(jnp.int32, (span, PAD), 1) == h
            cumc = jnp.sum(jnp.where(pick, cum_col[s], 0.0), axis=1, keepdims=True)
            beta = jnp.sum(jnp.where(pick, beta_col[s], 0.0), axis=1, keepdims=True)
            cumr = cum_row[s, pl.ds(h, 1), :]
            causal = row >= col
            weights = jnp.where(causal, jnp.exp(jnp.where(causal, cumc - cumr, 0.0)), 0.0)
            kb = k * beta
            kh = k.astype(bf16)
            lower = jnp.where(row > col, dot(kb.astype(bf16), kh, NT) * weights, 0.0)
            score = (dot(q.astype(bf16), kh, NT) * weights).astype(bf16)
            grow = jnp.exp(cumc)
            right = jnp.concatenate([v * beta, kb * grow], axis=1).astype(bf16)
            last = cumc[span - 1 :, :]
            kdec = (k * jnp.exp(last - cumc)).astype(bf16)
            each.append([lower, score, right, kdec, q * grow, jnp.exp(last)])
        unit = jnp.where(row == col, 1.0, 0.0)
        pair_mask = ((row >> 1) == (col >> 1)) & (row > col)
        inv = [unit - jnp.where(pair_mask, e[0], 0.0) for e in each]
        level = 1
        while (1 << level) < span:
            mask = ((row >> (level + 1)) == (col >> (level + 1))) & ((row >> level) > (col >> level))
            inv_h = [m.astype(bf16) for m in inv]
            mid = [
                dot(jnp.where(mask, e[0], 0.0).astype(bf16), m).astype(bf16)
                for e, m in zip(each, inv_h)
            ]
            inv = [m - dot(mh, t) for m, mh, t in zip(inv, inv_h, mid)]
            level += 1
        uw = [dot(m.astype(bf16), e[2]).astype(bf16) for m, e in zip(inv, each)]
        out = [dot(e[1], u) for e, u in zip(each, uw)]
        fin = [dot(e[3], u, TN) for e, u in zip(each, uw)]
        for p, e, o, z in zip(ps, each, out, fin):
            local_out[p] = o[:, :extent]
            reach[p] = (e[4] - o[:, extent:]).astype(bf16)
            step = (jnp.where(eye_lane, e[5] - 1.0, 0.0) - z[:, extent:]).astype(bf16)
            state = z[:, :extent].astype(bf16)

            @pl.when(p == me)
            def _():
                in_box[me, 0] = step
                in_box[me, 1] = state

            @pl.when(p != me)
            def _():
                out_box[p, 0] = step
                out_box[p, 1] = state
                send_box(p).start()

        return 0

    for s in range(seqs):
        project(s)
        lax.fori_loop(0, heads // group, functools.partial(local_group, s), 0)

    def back_copy(j):
        return pltpu.make_async_remote_copy(
            src_ref=back_out.at[j], dst_ref=back_in.at[me],
            send_sem=send2.at[j], recv_sem=recv2.at[me],
            device_id={"sp": j}, device_id_type=MESH,
        )

    def tail_copy(j):
        return pltpu.make_async_remote_copy(
            src_ref=tail_out.at[j], dst_ref=tail_in.at[me],
            send_sem=send3.at[j], recv_sem=recv3.at[me],
            device_id={"sp": j}, device_id_type=MESH,
        )

    @pl.when(me < pairs)
    def _():
        def chain(j, state):
            half = state.astype(bf16)

            @pl.when(j == me)
            def _():
                back_in[me] = half

            @pl.when(j != me)
            def _():
                back_out[j] = half
                back_copy(j).start()
                pltpu.make_async_remote_copy(
                    src_ref=out_box.at[0], dst_ref=in_box.at[j],
                    send_sem=send1.at[0], recv_sem=recv1.at[j],
                    device_id={"sp": j}, device_id_type=MESH,
                ).wait_recv()

            return state + dot(in_box[j, 0], half) + in_box[j, 1].astype(f32)

        final = lax.fori_loop(0, n, chain, jnp.zeros((extent, extent), f32))
        memory = final.astype(bf16).astype(f32)
        shape3 = nq_ref.shape
        mine = (
            lax.broadcasted_iota(jnp.int32, shape3, 0) * heads
            + lax.broadcasted_iota(jnp.int32, shape3, 1)
        ) == me

        def own(ref):
            kept = jnp.where(mine, ref[...].astype(f32), 0.0)
            return jnp.sum(jnp.sum(kept, axis=0), axis=0, keepdims=True)

        qn, kn = unit_rows(own(nq_ref)), unit_rows(own(nk_ref))
        both = jnp.concatenate([jnp.broadcast_to(qn, (PAD, extent)), jnp.broadcast_to(kn, (PAD, extent))], axis=0)
        reads = dot(both, memory, NN, highest)
        recall, retrieve = reads[0:1], reads[PAD : PAD + 1]
        s, h = me // heads, lax.rem(me, heads)
        beta_new, decay_new = nb_ref[s, h], nd_ref[s, h]
        fresh = own(nv_ref) - decay_new * retrieve
        meet = jnp.sum(kn * qn, axis=-1, keepdims=True)
        read = decay_new * recall + (beta_new * meet) * fresh
        norm = lax.rsqrt(jnp.mean(read * read, axis=-1, keepdims=True) + norm_floor)
        answer = jnp.broadcast_to(read * norm * gain_ref[...], (PAD, extent))
        for j in range(n):
            tail_out[j, 0:key_rows, :] = memory[j * key_rows : (j + 1) * key_rows]
            tail_out[j, tail_out.shape[1] - PAD :, :] = answer

        def push(j, _):
            @pl.when(j == me)
            def _():
                tail_in[me] = tail_out[me]

            @pl.when(j != me)
            def _():
                tail_copy(j).start()

            return 0

        lax.fori_loop(0, n, push, 0)

    gain = gain_ref[...]

    def finish(i, _):
        p = lax.rem(me + i, pairs)
        s, h = p // heads, lax.rem(p, heads)
        at = pl.ds(pl.multiple_of(s * span, span), span)
        lanes = pl.ds(pl.multiple_of(h * extent, extent), extent)

        @pl.when(p != me)
        def _():
            pltpu.make_async_remote_copy(
                src_ref=back_out.at[0], dst_ref=back_in.at[p],
                send_sem=send2.at[0], recv_sem=recv2.at[p],
                device_id={"sp": p}, device_id_type=MESH,
            ).wait_recv()

        o = local_out[p] + dot(reach[p], back_in[p])
        norm = lax.rsqrt(jnp.mean(o * o, axis=-1, keepdims=True) + norm_floor)
        gate = rows_ref[3, at, lanes].astype(f32)
        mixed_ref[at, lanes] = (o * norm * gain * (gate * jax.nn.sigmoid(gate))).astype(bf16)
        return 0

    lax.fori_loop(0, pairs, finish, 0)

    for p in range(pairs):

        @pl.when(p != me)
        def _():
            pltpu.make_async_remote_copy(
                src_ref=tail_out.at[0], dst_ref=tail_in.at[p],
                send_sem=send3.at[0], recv_sem=recv3.at[p],
                device_id={"sp": p}, device_id_type=MESH,
            ).wait_recv()

        cache_ref[p] = tail_in[p, 0:key_rows, :].astype(bf16)
        last = tail_in.shape[1]
        first_ref[p : p + 1, :] = tail_in[p, last - PAD : last - PAD + 1, :]

    for p in range(pairs):

        @pl.when(p != me)
        def _():
            send_box(p).wait_send()

    @pl.when(me < pairs)
    def _():
        for j in range(n):

            @pl.when(j != me)
            def _():
                back_copy(j).wait_send()
                tail_copy(j).wait_send()
    for s in range(seqs):
        for ck in range(chunks):
            part_copy(s, ck).wait_send()
            for d in range(1, chips):
                cross_copy(d, s, ck).wait_send()
                fwd_copy(d, s, ck).wait_send()


def run(n, tp, tokens, weights, bw, dw, bias, rate, gain, nq, nk, nv, nb, nd):
    seqs, span, kd = tokens.shape
    heads, depth = bw.shape
    width = weights[0].shape[1]
    rows, extent = seqs * span, width // heads
    pairs = seqs * heads
    chips = tp // 2
    kc = 256 if kd % 256 == 0 else kd
    chunks = kd // kc
    key_rows = extent // n
    tail = -(-key_rows // PAD) * PAD + PAD
    vmem = pl.BlockSpec(memory_space=pltpu.VMEM)
    smem = pl.BlockSpec(memory_space=pltpu.SMEM)
    hbm = pl.BlockSpec(memory_space=pl.ANY)
    return pl.pallas_call(
        functools.partial(kernel, n, tp, 2),
        out_shape=(
            jax.ShapeDtypeStruct((rows, width), bf16),
            jax.ShapeDtypeStruct((pairs, key_rows, extent), bf16),
            jax.ShapeDtypeStruct((pairs, extent), f32),
        ),
        in_specs=[hbm] * 5 + [vmem] * 2 + [smem] * 2 + [vmem] * 4 + [smem] * 2,
        out_specs=(vmem,) * 3,
        scratch_shapes=[
            pltpu.VMEM((seqs, span, kd), bf16),
            pltpu.VMEM((tp, seqs, chunks, span, kc), bf16),
            pltpu.VMEM((4, tp, kd, width), bf16),
            pltpu.VMEM((4, rows, width), f32),
            pltpu.VMEM((seqs, 2 * PAD, span), f32),
            pltpu.VMEM((2 * PAD, depth), bf16),
            pltpu.VMEM((4, rows, width), bf16),
            pltpu.VMEM((seqs, PAD, span), f32),
            pltpu.VMEM((seqs, span, PAD), f32),
            pltpu.VMEM((seqs, span, PAD), f32),
            pltpu.VMEM((pairs, span, extent), f32),
            pltpu.VMEM((pairs, span, extent), bf16),
            pltpu.VMEM((pairs, 2, extent, extent), bf16),
            pltpu.VMEM((n, 2, extent, extent), bf16),
            pltpu.VMEM((n, extent, extent), bf16),
            pltpu.VMEM((pairs, extent, extent), bf16),
            pltpu.VMEM((n, tail, extent), f32),
            pltpu.VMEM((pairs, tail, extent), f32),
            pltpu.SemaphoreType.DMA((seqs,)),
            pltpu.SemaphoreType.DMA((4, tp)),
            pltpu.SemaphoreType.DMA((chips - 1, seqs, chunks)),
            pltpu.SemaphoreType.DMA((seqs, chunks)),
            pltpu.SemaphoreType.DMA((chips - 1, seqs, chunks)),
            pltpu.SemaphoreType.DMA((tp, seqs, chunks)),
            pltpu.SemaphoreType.DMA((pairs,)),
            pltpu.SemaphoreType.DMA((n,)),
            pltpu.SemaphoreType.DMA((n,)),
            pltpu.SemaphoreType.DMA((pairs,)),
            pltpu.SemaphoreType.DMA((n,)),
            pltpu.SemaphoreType.DMA((pairs,)),
        ],
        compiler_params=pltpu.CompilerParams(
            collective_id=0, has_side_effects=True, vmem_limit_bytes=56 * 1024 * 1024
        ),
    )(tokens, *weights, bw, dw, bias, rate, gain, nq, nk, nv, nb, nd)


def shards(
    tokens, query_weight, key_weight, value_weight, gate_weight, beta_weight, decay_weight,
    beta_bias, rate_log, out_gain, new_query, new_key, new_value, new_beta, new_decay,
):
    seqs, span, kd = tokens.shape
    heads = rate_log.shape[0]
    extent = out_gain.shape[0]
    tp, sp = lax.axis_size("tp"), lax.axis_size("sp")
    weights = (query_weight, key_weight, value_weight, gate_weight)
    mixed, cache, first = run(
        sp, tp, tokens, weights, beta_weight.T, decay_weight.T, beta_bias, rate_log,
        out_gain[None], new_query, new_key, new_value, new_beta, new_decay,
    )
    return (
        mixed.reshape(seqs, span, heads * extent),
        cache.reshape(seqs, heads, extent // sp, extent),
        first.reshape(seqs, heads * extent),
    )


def solution(mesh):
    placed = (
        P(None, "sp", "tp"),
        P(None, "tp"),
        P(None, "tp"),
        P(None, "tp"),
        P(None, "tp"),
        P(None, "tp"),
        P(None, "tp"),
        P("tp"),
        P("tp"),
        P(),
        P(None, "tp", None),
        P(None, "tp", None),
        P(None, "tp", None),
        P(None, "tp"),
        P(None, "tp"),
    )
    return jax.shard_map(
        shards,
        mesh=mesh,
        in_specs=placed,
        out_specs=(P(None, "sp", "tp"), P(None, "tp", "sp", None), P(None, "tp")),
        check_vma=False,
    )
```

```python
import functools

import jax
import jax.numpy as jnp
from jax import lax
from jax.experimental import pallas as pl
from jax.experimental.pallas import tpu as pltpu
from jax.sharding import PartitionSpec as P

unit_floor = 1.0
norm_floor = 0.001
highest = lax.Precision.HIGHEST
MESH = pl.DeviceIdType.MESH
PAD = 8
f32 = jnp.float32
bf16 = jnp.bfloat16

NN = (((1,), (0,)), ((), ()))
NT = (((1,), (1,)), ((), ()))
TN = (((0,), (0,)), ((), ()))


def dot(left, right, dims=NN, precision=None):
    return lax.dot_general(left, right, dims, precision=precision, preferred_element_type=f32)


def gather_kernel(
    n, seqs, x_ref, wq_ref, wk_ref, wv_ref, wg_ref, bw_ref, dw_ref, out_ref,
    small_ref, bd_ref, xs, wbuf, acc, sacc, wsem, cross_sem, part_sem, fwd_sem, rx,
):
    me = lax.axis_index("tp")
    y, c = me // 2, lax.rem(me, 2)
    chips = n // 2
    rows, kd = x_ref.shape
    span = rows // seqs
    _, chunks, _, kc = xs.shape
    partner = y * 2 + (1 - c)
    weights = (wq_ref, wk_ref, wv_ref, wg_ref)

    barrier = pltpu.get_barrier_semaphore()
    pl.semaphore_signal(barrier, inc=1, device_id={"tp": partner}, device_id_type=MESH)
    for d in range(1, chips):
        to = lax.rem(y + d, chips) * 2 + c
        pl.semaphore_signal(barrier, inc=1, device_id={"tp": to}, device_id_type=MESH)

    order = [me, partner]
    for d in range(1, chips):
        source = lax.rem(y - d + chips, chips)
        order += [source * 2 + c, source * 2 + (1 - c)]

    def weight_copy(w, slot):
        start = pl.multiple_of(order[slot] * kd, kd)
        return pltpu.make_async_copy(
            weights[w].at[pl.ds(start, kd), :], wbuf.at[w, slot], wsem.at[w, slot]
        )

    for slot in range(n):
        for w in range(4):
            weight_copy(w, slot).start()
    bd_ref[...] = jnp.zeros_like(bd_ref)
    bd_ref[0 : bw_ref.shape[0]] = bw_ref[...]
    bd_ref[PAD : PAD + dw_ref.shape[0]] = dw_ref[...]
    pl.semaphore_wait(barrier, chips)

    def cols(ck):
        return pl.ds(ck * kc, kc)

    def cross_copy(d, ck):
        to = lax.rem(y + d, chips) * 2 + c
        return pltpu.make_async_remote_copy(
            src_ref=x_ref.at[:, cols(ck)], dst_ref=xs.at[me, ck],
            send_sem=cross_sem.at[d - 1, ck], recv_sem=rx.at[me, ck],
            device_id={"tp": to}, device_id_type=MESH,
        )

    def part_copy(ck):
        return pltpu.make_async_remote_copy(
            src_ref=x_ref.at[:, cols(ck)], dst_ref=xs.at[me, ck],
            send_sem=part_sem.at[ck], recv_sem=rx.at[me, ck],
            device_id={"tp": partner}, device_id_type=MESH,
        )

    def fwd_copy(d, ck):
        b = order[2 * d]
        return pltpu.make_async_remote_copy(
            src_ref=xs.at[b, ck], dst_ref=xs.at[b, ck],
            send_sem=fwd_sem.at[d - 1, ck], recv_sem=rx.at[b, ck],
            device_id={"tp": partner}, device_id_type=MESH,
        )

    def arrive(b, ck):
        pltpu.make_async_remote_copy(
            src_ref=xs.at[b, ck], dst_ref=xs.at[b, ck],
            send_sem=part_sem.at[ck], recv_sem=rx.at[b, ck],
            device_id={"tp": partner}, device_id_type=MESH,
        ).wait_recv()

    for ck in range(chunks):
        for d in range(1, chips):
            cross_copy(d, ck).start()
    for ck in range(chunks):
        part_copy(ck).start()

    def small(x, start, depth, first):
        piece = bd_ref[:, pl.ds(pl.multiple_of(start, depth), depth)]
        for s in range(seqs):
            term = dot(piece, x[s * span : (s + 1) * span], NT)
            sacc[s] = term if first else sacc[s] + term

    for w in range(4):
        weight_copy(w, 0).wait()
        acc[w] = dot(x_ref[...], wbuf[w, 0])
    small(x_ref[...], me * kd, kd, True)

    def use(slot, ck):
        b = order[slot]
        x = xs[b, ck]
        for w in range(4):
            if ck == 0:
                weight_copy(w, slot).wait()
            acc[w] += dot(x, wbuf[w, slot, pl.ds(ck * kc, kc), :])
        small(x, b * kd + ck * kc, kc, False)

    for ck in range(chunks):
        arrive(partner, ck)
        use(1, ck)
    for d in range(1, chips):
        for ck in range(chunks):
            arrive(order[2 * d], ck)
            fwd_copy(d, ck).start()
            use(2 * d, ck)
            arrive(order[2 * d + 1], ck)
            use(2 * d + 1, ck)
    for w in range(4):
        out_ref[w] = acc[w].astype(bf16)
    small_ref[...] = sacc[...]
    for ck in range(chunks):
        part_copy(ck).wait_send()
        for d in range(1, chips):
            cross_copy(d, ck).wait_send()
            fwd_copy(d, ck).wait_send()


def gather_project(n, seqs, tokens, weights, bw, dw):
    rows, kd = tokens.shape
    width = weights[0].shape[1]
    kc = 256 if kd % 256 == 0 else kd
    chunks = kd // kc
    chips = n // 2
    span = rows // seqs
    return pl.pallas_call(
        functools.partial(gather_kernel, n, seqs),
        out_shape=(
            jax.ShapeDtypeStruct((4, rows, width), bf16),
            jax.ShapeDtypeStruct((seqs, 2 * PAD, span), f32),
        ),
        in_specs=[pl.BlockSpec(memory_space=pltpu.VMEM)]
        + [pl.BlockSpec(memory_space=pl.ANY)] * 4
        + [pl.BlockSpec(memory_space=pltpu.VMEM)] * 2,
        out_specs=(pl.BlockSpec(memory_space=pltpu.VMEM),) * 2,
        scratch_shapes=[
            pltpu.VMEM((2 * PAD, bw.shape[1]), bf16),
            pltpu.VMEM((n, chunks, rows, kc), bf16),
            pltpu.VMEM((4, n, kd, width), bf16),
            pltpu.VMEM((4, rows, width), f32),
            pltpu.VMEM((seqs, 2 * PAD, span), f32),
            pltpu.SemaphoreType.DMA((4, n)),
            pltpu.SemaphoreType.DMA((chips - 1, chunks)),
            pltpu.SemaphoreType.DMA((chunks,)),
            pltpu.SemaphoreType.DMA((chips - 1, chunks)),
            pltpu.SemaphoreType.DMA((n, chunks)),
        ],
        compiler_params=pltpu.CompilerParams(
            collective_id=0, has_side_effects=True, vmem_limit_bytes=60 * 1024 * 1024
        ),
    )(tokens, *weights, bw, dw)


def unit_rows(values):
    return values * lax.rsqrt(jnp.sum(values * values, axis=-1, keepdims=True) + unit_floor)


def delta_kernel(
    n, seqs, heads, group, rows_ref, small_ref, bias_ref, rate_ref, gain_ref, nq_ref, nk_ref, nv_ref,
    nb_ref, nd_ref, mixed_ref, cache_ref, first_ref,
    cum_row, cum_col, beta_col, local_out, reach, out_box, in_box, back_out, back_in, tail_out,
    tail_in, send1, recv1, send2, recv2, send3, recv3,
):
    me = lax.axis_index("sp")
    pairs = seqs * heads
    span = rows_ref.shape[1] // seqs
    extent = rows_ref.shape[2] // heads
    key_rows = extent // n

    barrier = pltpu.get_barrier_semaphore()
    for d in range(1, n):
        to = lax.rem(me + d, n)
        pl.semaphore_signal(barrier, inc=1, device_id={"sp": to}, device_id_type=MESH)

    row = lax.broadcasted_iota(jnp.int32, (span, span), 0)
    col = lax.broadcasted_iota(jnp.int32, (span, span), 1)
    upper = jnp.where(row <= col, 1.0, 0.0)
    slot_of = lax.broadcasted_iota(jnp.int32, (PAD, 1), 0)
    bias = jnp.zeros((PAD, 1), f32)
    rate = jnp.zeros((PAD, 1), f32)
    for h in range(heads):
        bias = jnp.where(slot_of == h, bias_ref[h], bias)
        rate = jnp.where(slot_of == h, rate_ref[h], rate)
    for s in range(seqs):
        beta = jax.nn.sigmoid(small_ref[s, 0:PAD, :] + bias)
        pre = small_ref[s, PAD : 2 * PAD, :]
        soft = jnp.maximum(pre, 0.0) + jnp.log1p(jnp.exp(-jnp.abs(pre)))
        cum = dot(-jnp.exp(rate) * soft, upper, NN, highest)
        cum_row[s] = cum
        cum_col[s] = cum.T
        beta_col[s] = beta.T
    eye_lane = lax.broadcasted_iota(jnp.int32, (extent, extent), 0) == lax.broadcasted_iota(
        jnp.int32, (extent, extent), 1
    )
    pl.semaphore_wait(barrier, n - 1)

    def send_box(p):
        return pltpu.make_async_remote_copy(
            src_ref=out_box.at[p], dst_ref=in_box.at[me],
            send_sem=send1.at[p], recv_sem=recv1.at[me],
            device_id={"sp": p}, device_id_type=MESH,
        )

    def local_group(i, _):
        ps = [lax.rem(me + 1 + i * group + j, pairs) for j in range(group)]
        each = []
        for p in ps:
            s, h = p // heads, lax.rem(p, heads)
            at = pl.ds(pl.multiple_of(s * span, span), span)
            lanes = pl.ds(pl.multiple_of(h * extent, extent), extent)
            q = unit_rows(rows_ref[0, at, lanes].astype(f32))
            k = unit_rows(rows_ref[1, at, lanes].astype(f32))
            v = rows_ref[2, at, lanes].astype(f32)
            pick = lax.broadcasted_iota(jnp.int32, (span, PAD), 1) == h
            cumc = jnp.sum(jnp.where(pick, cum_col[s], 0.0), axis=1, keepdims=True)
            beta = jnp.sum(jnp.where(pick, beta_col[s], 0.0), axis=1, keepdims=True)
            cumr = cum_row[s, pl.ds(h, 1), :]
            causal = row >= col
            weights = jnp.where(causal, jnp.exp(jnp.where(causal, cumc - cumr, 0.0)), 0.0)
            kb = k * beta
            kh = k.astype(bf16)
            lower = jnp.where(row > col, dot(kb.astype(bf16), kh, NT) * weights, 0.0)
            score = (dot(q.astype(bf16), kh, NT) * weights).astype(bf16)
            grow = jnp.exp(cumc)
            right = jnp.concatenate([v * beta, kb * grow], axis=1).astype(bf16)
            last = cumc[span - 1 :, :]
            kdec = (k * jnp.exp(last - cumc)).astype(bf16)
            each.append([lower, score, right, kdec, q * grow, jnp.exp(last)])
        unit = jnp.where(row == col, 1.0, 0.0)
        pair_mask = ((row >> 1) == (col >> 1)) & (row > col)
        inv = [unit - jnp.where(pair_mask, e[0], 0.0) for e in each]
        level = 1
        while (1 << level) < span:
            mask = ((row >> (level + 1)) == (col >> (level + 1))) & ((row >> level) > (col >> level))
            inv_h = [m.astype(bf16) for m in inv]
            mid = [
                dot(jnp.where(mask, e[0], 0.0).astype(bf16), m).astype(bf16)
                for e, m in zip(each, inv_h)
            ]
            inv = [m - dot(mh, t) for m, mh, t in zip(inv, inv_h, mid)]
            level += 1
        uw = [dot(m.astype(bf16), e[2]).astype(bf16) for m, e in zip(inv, each)]
        out = [dot(e[1], u) for e, u in zip(each, uw)]
        fin = [dot(e[3], u, TN) for e, u in zip(each, uw)]
        for p, e, o, z in zip(ps, each, out, fin):
            local_out[p] = o[:, :extent]
            reach[p] = (e[4] - o[:, extent:]).astype(bf16)
            step = (jnp.where(eye_lane, e[5] - 1.0, 0.0) - z[:, extent:]).astype(bf16)
            state = z[:, :extent].astype(bf16)

            @pl.when(p == me)
            def _():
                in_box[me, 0] = step
                in_box[me, 1] = state

            @pl.when(p != me)
            def _():
                out_box[p, 0] = step
                out_box[p, 1] = state
                send_box(p).start()

        return 0

    lax.fori_loop(0, pairs // group, local_group, 0)

    def back_copy(j):
        return pltpu.make_async_remote_copy(
            src_ref=back_out.at[j], dst_ref=back_in.at[me],
            send_sem=send2.at[j], recv_sem=recv2.at[me],
            device_id={"sp": j}, device_id_type=MESH,
        )

    def tail_copy(j):
        return pltpu.make_async_remote_copy(
            src_ref=tail_out.at[j], dst_ref=tail_in.at[me],
            send_sem=send3.at[j], recv_sem=recv3.at[me],
            device_id={"sp": j}, device_id_type=MESH,
        )

    @pl.when(me < pairs)
    def _():
        def chain(j, state):
            half = state.astype(bf16)

            @pl.when(j == me)
            def _():
                back_in[me] = half

            @pl.when(j != me)
            def _():
                back_out[j] = half
                back_copy(j).start()
                pltpu.make_async_remote_copy(
                    src_ref=out_box.at[0], dst_ref=in_box.at[j],
                    send_sem=send1.at[0], recv_sem=recv1.at[j],
                    device_id={"sp": j}, device_id_type=MESH,
                ).wait_recv()

            return state + dot(in_box[j, 0], half) + in_box[j, 1].astype(f32)

        final = lax.fori_loop(0, n, chain, jnp.zeros((extent, extent), f32))
        memory = final.astype(bf16).astype(f32)
        shape3 = nq_ref.shape
        mine = (
            lax.broadcasted_iota(jnp.int32, shape3, 0) * heads
            + lax.broadcasted_iota(jnp.int32, shape3, 1)
        ) == me

        def own(ref):
            kept = jnp.where(mine, ref[...].astype(f32), 0.0)
            return jnp.sum(jnp.sum(kept, axis=0), axis=0, keepdims=True)

        qn, kn = unit_rows(own(nq_ref)), unit_rows(own(nk_ref))
        both = jnp.concatenate([jnp.broadcast_to(qn, (PAD, extent)), jnp.broadcast_to(kn, (PAD, extent))], axis=0)
        reads = dot(both, memory, NN, highest)
        recall, retrieve = reads[0:1], reads[PAD : PAD + 1]
        s, h = me // heads, lax.rem(me, heads)
        beta_new, decay_new = nb_ref[s, h], nd_ref[s, h]
        fresh = own(nv_ref) - decay_new * retrieve
        meet = jnp.sum(kn * qn, axis=-1, keepdims=True)
        read = decay_new * recall + (beta_new * meet) * fresh
        norm = lax.rsqrt(jnp.mean(read * read, axis=-1, keepdims=True) + norm_floor)
        answer = jnp.broadcast_to(read * norm * gain_ref[...], (PAD, extent))
        for j in range(n):
            tail_out[j, 0:key_rows, :] = memory[j * key_rows : (j + 1) * key_rows]
            tail_out[j, tail_out.shape[1] - PAD :, :] = answer

        def push(j, _):
            @pl.when(j == me)
            def _():
                tail_in[me] = tail_out[me]

            @pl.when(j != me)
            def _():
                tail_copy(j).start()

            return 0

        lax.fori_loop(0, n, push, 0)

    gain = gain_ref[...]

    def finish(i, _):
        p = lax.rem(me + i, pairs)
        s, h = p // heads, lax.rem(p, heads)
        at = pl.ds(pl.multiple_of(s * span, span), span)
        lanes = pl.ds(pl.multiple_of(h * extent, extent), extent)

        @pl.when(p != me)
        def _():
            pltpu.make_async_remote_copy(
                src_ref=back_out.at[0], dst_ref=back_in.at[p],
                send_sem=send2.at[0], recv_sem=recv2.at[p],
                device_id={"sp": p}, device_id_type=MESH,
            ).wait_recv()

        o = local_out[p] + dot(reach[p], back_in[p])
        norm = lax.rsqrt(jnp.mean(o * o, axis=-1, keepdims=True) + norm_floor)
        gate = rows_ref[3, at, lanes].astype(f32)
        mixed_ref[at, lanes] = (o * norm * gain * (gate * jax.nn.sigmoid(gate))).astype(bf16)
        return 0

    lax.fori_loop(0, pairs, finish, 0)

    for p in range(pairs):

        @pl.when(p != me)
        def _():
            pltpu.make_async_remote_copy(
                src_ref=tail_out.at[0], dst_ref=tail_in.at[p],
                send_sem=send3.at[0], recv_sem=recv3.at[p],
                device_id={"sp": p}, device_id_type=MESH,
            ).wait_recv()

        cache_ref[p] = tail_in[p, 0:key_rows, :].astype(bf16)
        last = tail_in.shape[1]
        first_ref[p : p + 1, :] = tail_in[p, last - PAD : last - PAD + 1, :]

    for p in range(pairs):

        @pl.when(p != me)
        def _():
            send_box(p).wait_send()

    @pl.when(me < pairs)
    def _():
        for j in range(n):

            @pl.when(j != me)
            def _():
                back_copy(j).wait_send()
                tail_copy(j).wait_send()


def delta(n, seqs, heads, rows4, small, bias, rate, gain, nq, nk, nv, nb, nd):
    _, rows, width = rows4.shape
    span, extent = rows // seqs, width // heads
    pairs = seqs * heads
    key_rows = extent // n
    tail = -(-key_rows // PAD) * PAD + PAD
    vmem = pl.BlockSpec(memory_space=pltpu.VMEM)
    smem = pl.BlockSpec(memory_space=pltpu.SMEM)
    return pl.pallas_call(
        functools.partial(delta_kernel, n, seqs, heads, 2),
        out_shape=(
            jax.ShapeDtypeStruct((rows, width), bf16),
            jax.ShapeDtypeStruct((pairs, key_rows, extent), bf16),
            jax.ShapeDtypeStruct((pairs, extent), f32),
        ),
        in_specs=[vmem] * 2 + [smem] * 2 + [vmem] * 4 + [smem] * 2,
        out_specs=(vmem,) * 3,
        scratch_shapes=[
            pltpu.VMEM((seqs, PAD, span), f32),
            pltpu.VMEM((seqs, span, PAD), f32),
            pltpu.VMEM((seqs, span, PAD), f32),
            pltpu.VMEM((pairs, span, extent), f32),
            pltpu.VMEM((pairs, span, extent), bf16),
            pltpu.VMEM((pairs, 2, extent, extent), bf16),
            pltpu.VMEM((n, 2, extent, extent), bf16),
            pltpu.VMEM((n, extent, extent), bf16),
            pltpu.VMEM((pairs, extent, extent), bf16),
            pltpu.VMEM((n, tail, extent), f32),
            pltpu.VMEM((pairs, tail, extent), f32),
            pltpu.SemaphoreType.DMA((pairs,)),
            pltpu.SemaphoreType.DMA((n,)),
            pltpu.SemaphoreType.DMA((n,)),
            pltpu.SemaphoreType.DMA((pairs,)),
            pltpu.SemaphoreType.DMA((n,)),
            pltpu.SemaphoreType.DMA((pairs,)),
        ],
        compiler_params=pltpu.CompilerParams(
            collective_id=1, has_side_effects=True, vmem_limit_bytes=48 * 1024 * 1024
        ),
    )(rows4, small, bias, rate, gain, nq, nk, nv, nb, nd)


def shards(
    tokens, query_weight, key_weight, value_weight, gate_weight, beta_weight, decay_weight,
    beta_bias, rate_log, out_gain, new_query, new_key, new_value, new_beta, new_decay,
):
    seqs, span, kd = tokens.shape
    heads = rate_log.shape[0]
    extent = out_gain.shape[0]
    tp, sp = lax.axis_size("tp"), lax.axis_size("sp")
    weights = (query_weight, key_weight, value_weight, gate_weight)
    rows4, small = gather_project(tp, seqs, tokens.reshape(seqs * span, kd), weights, beta_weight.T, decay_weight.T)
    mixed, cache, first = delta(
        sp, seqs, heads, rows4, small, beta_bias, rate_log, out_gain[None], new_query, new_key, new_value,
        new_beta, new_decay,
    )
    return (
        mixed.reshape(seqs, span, heads * extent),
        cache.reshape(seqs, heads, extent // sp, extent),
        first.reshape(seqs, heads * extent),
    )


def solution(mesh):
    placed = (
        P(None, "sp", "tp"),
        P(None, "tp"),
        P(None, "tp"),
        P(None, "tp"),
        P(None, "tp"),
        P(None, "tp"),
        P(None, "tp"),
        P("tp"),
        P("tp"),
        P(),
        P(None, "tp", None),
        P(None, "tp", None),
        P(None, "tp", None),
        P(None, "tp"),
        P(None, "tp"),
    )
    return jax.shard_map(
        shards,
        mesh=mesh,
        in_specs=placed,
        out_specs=(P(None, "sp", "tp"), P(None, "tp", "sp", None), P(None, "tp")),
        check_vma=False,
    )
```
